256 devices in a mesh: ep: 16 (over y, x), tp: 16 (over z, core).
Axes of the slice: x: 4, y: 4, z: 8, core: 2. Of those that a mesh axis runs over, the one named last changes fastest.
Arguments:
- mix_in: bfloat16 [32768, 2048], P(('ep', 'tp')), may hold values from -6 to 6
- mix_gain: float32 [2048], replicated, may hold values from 0.1 to 1.9
- mix_w_in: bfloat16 [2048, 512], P('tp'), may hold values from -0.125 to 0.125
- pool_mat: bfloat16 [4, 128, 128], replicated, may hold values from -0.5 to 0.5
- pool_scale: float32 [512], replicated, may hold values from 0.1 to 1.9
- mix_w_out: bfloat16 [512, 2048], P(None, 'tp'), may hold values from -0.25 to 0.25
- moe_in: bfloat16 [32768, 2048], P(('ep', 'tp')), may hold values from -6 to 6
- moe_gain: float32 [2048], replicated, may hold values from 0.1 to 1.9
- routes: int32 [32768, 2], P('ep'), may hold values from 0 to 255, all different within a row; in each aligned block of 2048 rows (0 to 2047, 2048 to 4095, ...) at most 32 rows name the same one
- route_score: bfloat16 [32768, 2], P('ep'), may hold values from 0.099609375 to 1
- exp_gate: bfloat16 [256, 2048, 768], P(('ep', 'tp')), may hold values from -0.125 to 0.125
- exp_up: bfloat16 [256, 2048, 768], P(('ep', 'tp')), may hold values from -0.125 to 0.125
- exp_down: bfloat16 [256, 768, 2048], P(('ep', 'tp')), may hold values from -0.21875 to 0.21875
- shared_gate: bfloat16 [768, 2048], P('tp'), may hold values from -0.125 to 0.125
- shared_up: bfloat16 [768, 2048], P('tp'), may hold values from -0.125 to 0.125
- shared_down: bfloat16 [768, 2048], P('tp'), may hold values from -0.21875 to 0.21875
Outputs:
- mixed: bfloat16 [32768, 2048], P(('ep', 'tp'))
- moe_out: bfloat16 [32768, 2048], P(('ep', 'tp'))
The draws below stay inside these ranges and needn't reach their ends.
Inputs may be any that keep to these rules, and one draw needn't show every extreme that they name: `routes`: each row names 2 different experts. Within the rows of one index of ep (aligned blocks of 2048 rows) no expert is named more than 32 times, a bound that some expert reaches in some blocks.
All inputs are finite; a program needn't handle non-finite values.
Results may differ from the reference program's by a relative error of at most 0.012.
Values may be sent and summed in bfloat16 or wider, within the bound.
No kernel may reach another device: no remote copies, remote signals or barrier semaphores. Data moves between devices by JAX's collectives and lax.ppermute only.
A program may use at most 128 MiB of HBM per device.

```python
import math
import jax
import jax.numpy as jnp
import numpy as np
from jax import lax

D = 2048
GROUP_CH = 128
POOL_GROUPS = 4
POOL = 512
FF = 768
FF_SH = 768
TOP_K = 2
SEQS_MIX = 1
TOK_MOE = 128
EXPERTS = 256
CAP = 32
TOKENS_MIX = 32768
LEN_MIX = 32768
TOKENS_MOE = 32768
N_EP = 16
N_TP = 16


def shard_levels(own_key, shape, shards, low, high):
    def one(axis_at, blocks):
        draws = jax.random.uniform(jax.random.fold_in(jax.random.fold_in(own_key, 6), axis_at), (blocks,), jnp.float32, low / len(shards), high / len(shards))
        return jnp.repeat(jnp.exp(draws), shape[axis_at] // blocks).reshape((-1,) + (1,) * (len(shape) - axis_at - 1))

    level = one(*shards[0])
    for cut in shards[1:]:
        level = level * one(*cut)
    return level


def deal_out(key, own, number, rows, number_of, top, reach, lean):
    sequence = jax.random.permutation(key, number_of)
    crowded, common = portions_of(number_of, rows * top, reach, lean, True), portions_of(number_of, rows * top, reach, lean, False)
    places = jnp.arange(number_of)

    def named(sizes, turn):
        used = int((sizes > 0).sum())
        fixed = max(1, used // 4)
        shifted = fixed + (places - fixed + turn * (used - fixed)) % max(1, number_of - fixed)
        return jnp.zeros((number_of,), jnp.int32).at[sequence[jnp.where(places < fixed, places, shifted)]].set(jnp.asarray(sizes, jnp.int32))

    sizes = jnp.where(number % 4 == 0, named(crowded, number // 4), named(common, number - number // 4 - 1))
    mixed = jax.random.permutation(jax.random.fold_in(own, 3), number_of)
    donor, taker = mixed[0:number_of // 2 * 2:2], mixed[1:number_of // 2 * 2:2]
    margin = jnp.minimum(sizes[donor] - 1, reach - sizes[taker]) // 2
    margin = jnp.where((donor == sequence[0]) | (taker == sequence[0]) | (sizes[taker] == 0), 0, jnp.maximum(margin, 0))
    shifted = jax.random.randint(jax.random.fold_in(own, 4), (number_of // 2,), 0, 1 << 20) % (margin + 1)
    sizes = sizes.at[donor].add(-shifted).at[taker].add(shifted)
    labels = jnp.searchsorted(jnp.cumsum(sizes), jnp.arange(rows * top), side="right").astype(jnp.int32)
    grid = labels.reshape(top, rows).T
    grid = grid[jax.random.permutation(jax.random.fold_in(own, 1), rows)]
    turn = jax.random.randint(jax.random.fold_in(own, 2), (rows, 1), 0, top)
    return jnp.take_along_axis(grid, (jnp.arange(top)[None, :] + turn) % top, axis=1)


def portions_of(amount, total, most, slope, full):
    weights = [(1 << 20) // math.isqrt(rank ** slope) + 1 for rank in range(1, amount + 1)]
    largest = most if full else min(most, max(-(-total // amount), total * weights[0] // sum(weights)))
    least = 1 if total - largest >= amount - 1 else 0
    given, surplus = [largest] + [least] * (amount - 1), total - largest - least * (amount - 1)
    while surplus > 0:
        candidates = [i for i in range(1, amount) if given[i] < largest] or [i for i in range(1, amount) if given[i] < most]
        mass, budget = sum([weights[i] for i in candidates]), surplus
        for i in candidates:
            addition = min(most - given[i], max(1, budget * weights[i] // mass), surplus)
            given[i] = given[i] + addition
            surplus = surplus - addition
    return np.array(given)


def normal_values(rng, shape, spread, most, split=(), kind=jnp.bfloat16):
    array = spread * jax.random.normal(rng, shape, jnp.float32)
    if split:
        array = array * shard_levels(rng, shape, split, -0.22, 0.18)
    return jnp.clip(array, -most, most).astype(kind)


def setup_inputs(seed: int = 0) -> dict:
    arg_keys = jax.random.split(jax.random.key(seed), 17)
    mix_in = normal_values(arg_keys[0], (TOKENS_MIX, D), 1.0, 6.0, ((0, 256),))
    mix_gain = jnp.clip(1.0 + 0.18 * jax.random.normal(arg_keys[1], (D,), jnp.float32), 0.1, 1.9)
    mix_w_in = normal_values(arg_keys[2], (D, POOL), D ** -0.5, 0.125, ((0, 16),))
    pool_mat = normal_values(arg_keys[3], (POOL_GROUPS, GROUP_CH, GROUP_CH), GROUP_CH ** -0.5, 0.5)
    pool_scale = jnp.clip(1.0 + 0.18 * jax.random.normal(arg_keys[4], (POOL,), jnp.float32), 0.1, 1.9)
    mix_w_out = normal_values(arg_keys[5], (POOL, D), POOL ** -0.5, 0.25, ((1, 16),))
    moe_in = normal_values(arg_keys[6], (TOKENS_MOE, D), 1.0, 6.0, ((0, 256),))
    moe_gain = jnp.clip(1.0 + 0.18 * jax.random.normal(arg_keys[7], (D,), jnp.float32), 0.1, 1.9)
    routes_keys = jax.random.split(jax.random.fold_in(arg_keys[8], 1), TOKENS_MOE // (TOK_MOE * N_TP))
    routes_turns = jax.random.permutation(jax.random.fold_in(arg_keys[8], 3), TOKENS_MOE // (TOK_MOE * N_TP))
    routes = jax.vmap(lambda own, number: deal_out(jax.random.fold_in(arg_keys[8], 2), own, number, TOK_MOE * N_TP, EXPERTS, TOP_K, CAP, 2))(routes_keys, routes_turns).reshape((TOKENS_MOE, TOP_K))
    route_score = jnp.clip(jnp.exp(math.log(1.0) - 2.306499 * jax.random.uniform(arg_keys[9], (TOKENS_MOE, TOP_K), jnp.float32) ** shard_levels(arg_keys[9], (TOKENS_MOE, TOP_K), ((0, 16),), -0.2, 0.2)), 0.099609375, 1.0).astype(jnp.bfloat16)
    exp_gate = normal_values(arg_keys[10], (EXPERTS, D, FF), D ** -0.5, 0.125, ((0, 256),))
    exp_up = normal_values(arg_keys[11], (EXPERTS, D, FF), D ** -0.5, 0.125, ((0, 256),))
    exp_down = normal_values(arg_keys[12], (EXPERTS, FF, D), FF ** -0.5, 0.21875, ((0, 256),))
    shared_gate = normal_values(arg_keys[13], (FF_SH, D), D ** -0.5, 0.125, ((0, 16),))
    shared_up = normal_values(arg_keys[14], (FF_SH, D), D ** -0.5, 0.125, ((0, 16),))
    shared_down = normal_values(arg_keys[15], (FF_SH, D), FF_SH ** -0.5, 0.21875, ((0, 16),))
    return dict(mix_in=mix_in, mix_gain=mix_gain, mix_w_in=mix_w_in, pool_mat=pool_mat, pool_scale=pool_scale, mix_w_out=mix_w_out, moe_in=moe_in, moe_gain=moe_gain, routes=routes, route_score=route_score, exp_gate=exp_gate, exp_up=exp_up, exp_down=exp_down, shared_gate=shared_gate, shared_up=shared_up, shared_down=shared_down)


NORM_EPS = 1e-06
ROUTED_SCALE = 2.5

def rms_rows(values, gain):
    floats = values.astype(jnp.float32)
    scaled = floats * lax.rsqrt(lax.optimization_barrier(jnp.mean(floats * floats, axis=-1, keepdims=True)) + NORM_EPS)
    return (scaled * gain.astype(jnp.float32)).astype(jnp.bfloat16)

def expert_ffn(rows_in, w_gate, w_up, w_down):
    gate_act = jnp.dot(rows_in, w_gate, preferred_element_type=jnp.float32)
    up_act = jnp.dot(rows_in, w_up, preferred_element_type=jnp.float32)
    hidden = (jax.nn.silu(gate_act) * up_act).astype(jnp.bfloat16)
    return jnp.dot(hidden, w_down, preferred_element_type=jnp.float32).astype(jnp.bfloat16)

def mixer_ref(mix_in, mix_gain, mix_w_in, pool_mat, pool_scale, mix_w_out):
    normed = rms_rows(mix_in, mix_gain)
    projected = jnp.dot(normed, mix_w_in, preferred_element_type=jnp.float32).astype(jnp.bfloat16)
    channels = projected.shape[1]
    reach_rows = 2 ** POOL_GROUPS - 1
    floats = projected.astype(jnp.float32).reshape(SEQS_MIX, LEN_MIX, channels)
    padded = jnp.pad(floats, ((0, 0), (reach_rows, 0), (0, 0)))
    position = jnp.arange(LEN_MIX, dtype=jnp.int32)
    pieces = []
    for group in range(POOL_GROUPS):
        window_len = 2 ** (group + 1)
        lower = group * GROUP_CH
        upper = lower + GROUP_CH
        running = jnp.zeros((SEQS_MIX, LEN_MIX, GROUP_CH), jnp.float32)
        for offset in range(window_len):
            running = running + padded[:, reach_rows - offset:reach_rows - offset + LEN_MIX, lower:upper]
        counts = jnp.minimum(position + 1, window_len).astype(jnp.float32)
        pieces.append(running / counts[None, :, None] - floats[:, :, lower:upper])
    pooled = jnp.concatenate(pieces, axis=2).astype(jnp.bfloat16).reshape(-1, POOL_GROUPS, GROUP_CH)
    grouped = jnp.einsum('tgc,gcd->tgd', pooled.astype(jnp.float32), pool_mat.astype(jnp.float32))
    pool_out = (grouped.reshape(-1, channels) * pool_scale).astype(jnp.bfloat16)
    return jnp.dot(pool_out, mix_w_out, preferred_element_type=jnp.float32).astype(jnp.bfloat16)

def experts_ref(moe_in, moe_gain, routes, route_score, exp_gate, exp_up, exp_down, shared_gate, shared_up, shared_down):
    normed = rms_rows(moe_in, moe_gain)
    total_rows, model_width = normed.shape
    block_rows = TOK_MOE * N_TP
    per_block = block_rows * TOP_K
    scores = route_score.astype(jnp.float32)
    weights = scores / lax.optimization_barrier(jnp.sum(scores, axis=1, keepdims=True)) * ROUTED_SCALE
    flat_expert = routes.reshape(N_EP, per_block)
    onehot = (flat_expert[:, :, None] == jnp.arange(EXPERTS, dtype=jnp.int32)[None, None, :]).astype(jnp.int32)
    before = lax.optimization_barrier(jnp.sum((jnp.cumsum(onehot, axis=1) - onehot) * onehot, axis=2))
    block_id = jnp.arange(N_EP, dtype=jnp.int32)[:, None]
    slot_span = N_EP * CAP
    flat_slot = (flat_expert * slot_span + block_id * CAP + before).reshape(-1).astype(jnp.int32)
    token_id = (block_id * block_rows + jnp.arange(per_block, dtype=jnp.int32)[None, :] // TOP_K).reshape(-1)
    table = jnp.full((EXPERTS * slot_span,), total_rows, jnp.int32).at[flat_slot].set(token_id)
    table = table.reshape(EXPERTS, slot_span)
    table_weight = jnp.zeros((EXPERTS * slot_span,), jnp.float32).at[flat_slot].set(weights.reshape(-1))
    table_weight = table_weight.reshape(EXPERTS, slot_span)
    padded_rows = jnp.concatenate([normed, jnp.zeros((1, model_width), jnp.bfloat16)], axis=0)
    gate_act = jnp.dot(normed, shared_gate.T, preferred_element_type=jnp.float32)
    up_act = jnp.dot(normed, shared_up.T, preferred_element_type=jnp.float32)
    shared_hidden = (jax.nn.silu(gate_act) * up_act).astype(jnp.bfloat16)
    shared_out = jnp.dot(shared_hidden, shared_down, preferred_element_type=jnp.float32)

    def column_sum(running, column):

        def one_expert(partial_value, ep_rank):
            expert = ep_rank * N_TP + column
            ids = table[expert]
            rows_in = jnp.take(padded_rows, ids, axis=0)
            outputs = expert_ffn(rows_in, exp_gate[expert], exp_up[expert], exp_down[expert])
            partial_value = partial_value.at[ids].add(outputs.astype(jnp.float32) * table_weight[expert][:, None], mode='drop')
            return (partial_value, None)
        partial_value = jnp.zeros((total_rows, model_width), jnp.float32)
        partial_value, _ = lax.scan(one_expert, partial_value, jnp.arange(N_EP, dtype=jnp.int32))
        return (running + partial_value.astype(jnp.bfloat16).astype(jnp.float32), None)
    running, _ = lax.scan(column_sum, jnp.zeros((total_rows, model_width), jnp.float32), jnp.arange(N_TP, dtype=jnp.int32))
    return (running + shared_out).astype(jnp.bfloat16)

def reference(mix_in, mix_gain, mix_w_in, pool_mat, pool_scale, mix_w_out, moe_in, moe_gain, routes, route_score, exp_gate, exp_up, exp_down, shared_gate, shared_up, shared_down):
    mixed = mixer_ref(mix_in, mix_gain, mix_w_in, pool_mat, pool_scale, mix_w_out)
    moe_out = experts_ref(moe_in, moe_gain, routes, route_score, exp_gate, exp_up, exp_down, shared_gate, shared_up, shared_down)
    return (mixed, moe_out)
```

```python
import jax
import jax.numpy as jnp
from jax import lax
from jax.experimental import pallas as pl
from jax.experimental.pallas import tpu as pltpu
from jax.sharding import PartitionSpec as P


SEQS_MIX = 1

NORM_EPS = 1e-06
ROUTED_SCALE = 2.5


F32 = jnp.float32
BF16 = jnp.bfloat16


def shifted(value, axis, steps):
    count = lax.axis_size(axis)
    first, last = (max(0, -steps), min(count, count - steps))
    return lax.ppermute(value, axis, [(source, source + steps) for source in range(first, last)])


def after(value, *earlier):
    return lax.optimization_barrier((value,) + earlier)[0]


def rms_rows(values, gain):
    floats = values.astype(F32)
    scaled = floats * lax.rsqrt(jnp.mean(floats * floats, axis=-1, keepdims=True) + NORM_EPS)
    return (scaled * gain).astype(BF16)


def to_next(value):
    count = lax.axis_size("tp")
    return lax.ppermute(value, "tp", [(t, (t + 2) % count) for t in range(count)])


def to_prev(value):
    count = lax.axis_size("tp")
    return lax.ppermute(value, "tp", [(t, (t - 2) % count) for t in range(count)])


def to_partner(value):
    count = lax.axis_size("tp")
    return lax.ppermute(value, "tp", [(t, t ^ 1) for t in range(count)])


def exchanged(value):
    return lax.all_to_all(value, "ep", split_axis=0, concat_axis=0, tiled=True)


def ring_gather(own):
    chips = lax.axis_size("tp") // 2
    far = chips // 2
    half = own.shape[0] // 2
    pieces = [None] * chips
    pieces[0] = own
    ahead, behind = own, own
    for step in range(1, far):
        behind = to_next(behind)
        ahead = to_prev(ahead)
        pieces[chips - step] = behind
        pieces[step] = ahead
    pieces[far] = (to_next(behind[:half]), to_prev(ahead[half:]))
    return pieces


def ring_visits(chips):
    far = chips // 2
    order = [far]
    for step in range(far - 1, 0, -1):
        order += [step, chips - step]
    return order + [0]


def vmem_spec():
    return pl.BlockSpec(memory_space=pltpu.VMEM)


def smem_spec():
    return pl.BlockSpec(memory_space=pltpu.SMEM)


def aligned(index, block):
    return pl.ds(pl.multiple_of(index * block, block), block)


def select_rows(select, pieces):
    flat = []
    places = []
    rows = 0
    cols = pieces[0].shape[1]
    for place in ring_visits(len(pieces)):
        piece = pieces[place]
        for part in piece if isinstance(piece, tuple) else (piece,):
            flat.append(part)
            places.append((rows, part.shape[0]))
            rows += part.shape[0]
    picks = select.shape[0]

    def body(select_ref, *refs):
        part_refs = refs[: len(flat)]
        rows_ref, picked_ref = refs[len(flat) :]
        for ref, (row, height) in zip(part_refs, places):
            rows_ref[row : row + height, :] = ref[...]

        @pl.loop(0, cols // 256)
        def _(c):
            across = aligned(c, 256)
            picked_ref[:, across] = jnp.dot(
                select_ref[...], rows_ref[:, across], preferred_element_type=F32
            ).astype(BF16)

    return pl.pallas_call(
        body,
        name="select_rows",
        out_shape=(
            jax.ShapeDtypeStruct((rows, cols), BF16),
            jax.ShapeDtypeStruct((picks, cols), BF16),
        ),
        in_specs=[vmem_spec()] * (1 + len(flat)),
        out_specs=(vmem_spec(), vmem_spec()),
        cost_estimate=pl.CostEstimate(
            flops=2 * picks * rows * cols,
            bytes_accessed=2 * (picks * rows + 2 * rows * cols + picks * cols),
            transcendentals=0,
        ),
    )(select, *flat)


def stack_rows(arrays):
    rows = sum(a.shape[0] for a in arrays)
    cols = arrays[0].shape[1]

    def body(*refs):
        row = 0
        for ref in refs[:-1]:
            refs[-1][row : row + ref.shape[0], :] = ref[...]
            row += ref.shape[0]

    return pl.pallas_call(
        body,
        name="stack_rows",
        out_shape=jax.ShapeDtypeStruct((rows, cols), arrays[0].dtype),
        in_specs=[vmem_spec()] * len(arrays),
        out_specs=vmem_spec(),
        cost_estimate=pl.CostEstimate(
            flops=rows * cols, bytes_accessed=4 * rows * cols, transcendentals=0
        ),
    )(*arrays)


def add_received(total, places, received, height, from_rows):
    width = total.shape[1]
    count = len(places)

    def body(*refs):
        strips, arrivals, outs = refs[:count], refs[count : 2 * count], refs[2 * count :]
        for strip, arrival, out, row in zip(strips, arrivals, outs, from_rows):
            rows = slice(row, row + arrival.shape[0])
            if arrival.shape[0] < height:
                out[...] = strip[...]
            out[rows, :] = (strip[rows, :].astype(F32) + arrival[...].astype(F32)).astype(BF16)

    def strip_at(place):
        return pl.BlockSpec((height, width), lambda i: (place, 0))

    def whole(array):
        return pl.BlockSpec(array.shape, lambda i: (0, 0))

    return pl.pallas_call(
        body,
        grid=(1,),
        out_shape=tuple(jax.ShapeDtypeStruct((height, width), BF16) for _ in places),
        in_specs=[strip_at(p) for p in places] + [whole(r) for r in received],
        out_specs=tuple(strip_at(0) for _ in places),
        cost_estimate=pl.CostEstimate(
            flops=count * height * width,
            bytes_accessed=6 * count * height * width,
            transcendentals=0,
        ),
    )(*[total] * count, *received)


def ring_scatter(totals, strip, height):
    chips = lax.axis_size("tp") // 2
    far = chips // 2
    half = height // 2
    early, late = totals
    start = early[strip * height : (strip + 1) * height]
    up = to_next(start[:half])
    down = to_prev(start[half:])
    for step in range(2, far + 1):
        total, at = (early, 1) if step == 2 else (late, 2 * (step - 3))
        places = [2 * at + strip, 2 * (at + 1) + strip]
        rows = (0, half) if step == 2 else (0, 0)
        up, down = add_received(total, places, (up, down), height, rows)
        up = to_next(up)
        down = to_prev(down)
    return up, down


def last_sums(late, arrivals, height):
    width = late.shape[1]
    strips = len(arrivals)
    block = strips * height

    def body(own_ref, *refs):
        out_ref = refs[-1]
        for h in range(strips):
            rows = slice(h * height, (h + 1) * height)
            total = own_ref[rows, :].astype(F32)
            total += refs[2 * h][...].astype(F32)
            total += refs[2 * h + 1][...].astype(F32)
            out_ref[rows, :] = total.astype(BF16)

    place = late.shape[0] // block - 1
    flat = [a for pair in arrivals for a in pair]
    return pl.pallas_call(
        body,
        name="last_sums",
        grid=(1,),
        out_shape=jax.ShapeDtypeStruct((block, width), BF16),
        in_specs=[pl.BlockSpec((block, width), lambda i: (place, 0))]
        + [pl.BlockSpec(a.shape, lambda i: (0, 0)) for a in flat],
        out_specs=pl.BlockSpec((block, width), lambda i: (0, 0)),
        cost_estimate=pl.CostEstimate(
            flops=2 * block * width, bytes_accessed=8 * block * width, transcendentals=0
        ),
    )(late, *flat)


def joined_sums(lefts, rights):
    rows, cols = lefts[0].shape
    count = len(lefts)

    def body(*refs):
        for f in range(count):
            refs[-1][:, f * cols : (f + 1) * cols] = refs[f][...] + refs[count + f][...]

    block = rows // 4
    spec = pl.BlockSpec((block, cols), lambda i: (i, 0))
    return pl.pallas_call(
        body,
        name="joined_sums",
        grid=(4,),
        out_shape=jax.ShapeDtypeStruct((rows, count * cols), BF16),
        in_specs=[spec] * (2 * count),
        out_specs=pl.BlockSpec((block, count * cols), lambda i: (i, 0)),
        cost_estimate=pl.CostEstimate(
            flops=rows * cols * count, bytes_accessed=6 * rows * cols * count, transcendentals=0
        ),
    )(*lefts, *rights)


def project_rows(position, normed, own, other, channels):
    tokens = normed.shape[0]
    block = 128
    chips = own.shape[0] // block

    def body(position_ref, normed_ref, own_ref, other_ref, out_ref):
        chip, core = position_ref[0], position_ref[1]

        def step(place, total):
            at = 2 * ((chip + place) % chips)
            rows = aligned(place, block)
            for ref, turn in ((own_ref, core), (other_ref, 1 - core)):
                total += jnp.dot(
                    normed_ref[:, aligned(at + turn, block)],
                    ref[rows, :channels],
                    preferred_element_type=F32,
                )
            return total

        total = lax.fori_loop(0, chips, step, jnp.zeros((tokens, channels), F32))
        out_ref[...] = total.astype(BF16)

    return pl.pallas_call(
        body,
        name="project_rows",
        out_shape=jax.ShapeDtypeStruct((tokens, channels), BF16),
        in_specs=[smem_spec()] + [vmem_spec()] * 3,
        out_specs=vmem_spec(),
        cost_estimate=pl.CostEstimate(
            flops=2 * tokens * normed.shape[1] * channels,
            bytes_accessed=2 * (normed.size + own.size + other.size),
            transcendentals=0,
        ),
    )(position, normed, own, other)


def output_rows(position, pool_out, own, other):
    tokens, channels = pool_out.shape
    block = 128
    chips = own.shape[0] // block
    groups = channels // block

    def body(position_ref, pool_ref, own_ref, other_ref, out_ref):
        chip, core = position_ref[0], position_ref[1]

        @pl.loop(0, chips)
        def _(place):
            at = 2 * ((chip + place) % chips)
            rows = aligned(place, block)
            for ref, turn in ((own_ref, core), (other_ref, 1 - core)):
                matrix = jnp.concatenate(
                    [
                        ref[rows, channels + g * block : channels + (g + 1) * block]
                        for g in range(groups)
                    ],
                    axis=0,
                )
                out_ref[:, aligned(at + turn, block)] = jnp.dot(
                    pool_ref[...], matrix, preferred_element_type=F32
                ).astype(BF16)

    return pl.pallas_call(
        body,
        name="output_rows",
        out_shape=jax.ShapeDtypeStruct((tokens, 2 * chips * block), BF16),
        in_specs=[smem_spec()] + [vmem_spec()] * 3,
        out_specs=vmem_spec(),
        cost_estimate=pl.CostEstimate(
            flops=4 * tokens * chips * block * channels,
            bytes_accessed=2 * (own.size + other.size),
            transcendentals=0,
        ),
    )(position, pool_out, own, other)


def pool_mix(projected, prior_tail, first_row, seq_len, pool_mat, pool_scale):
    tokens, channels = projected.shape
    groups = pool_mat.shape[0]
    group_ch = pool_mat.shape[1]
    reach_rows = prior_tail.shape[0]
    extended = jnp.concatenate([prior_tail, projected], axis=0).astype(F32)
    prefix = jnp.concatenate(
        [jnp.zeros((1, channels), F32), jnp.cumsum(extended, axis=0)], axis=0
    )
    position = (first_row + lax.iota(jnp.int32, tokens)) % seq_len
    pieces = []
    for group in range(groups):
        window_len = 2 ** (group + 1)
        lower = group * group_ch
        upper = lower + group_ch
        window_sum = (
            prefix[reach_rows + 1 : reach_rows + 1 + tokens, lower:upper]
            - prefix[
                reach_rows + 1 - window_len : reach_rows + 1 - window_len + tokens, lower:upper
            ]
        )
        counts = jnp.minimum(position + 1, window_len).astype(F32)
        pieces.append(window_sum / counts[:, None] - extended[reach_rows:, lower:upper])
    pooled = jnp.concatenate(pieces, axis=1).astype(BF16).reshape(tokens, groups, group_ch)
    grouped = jnp.einsum("tgc,gcd->tgd", pooled, pool_mat, preferred_element_type=F32)
    return (grouped.reshape(tokens, channels) * pool_scale).astype(BF16)


def strict_upper(size):
    row = lax.broadcasted_iota(jnp.int32, (size, size), 0)
    col = lax.broadcasted_iota(jnp.int32, (size, size), 1)
    return (row < col).astype(BF16)


def slot_tables(routes, route_score, chip, core, capacity):
    block_rows, top_count = routes.shape
    ep_count = lax.axis_size("ep")
    tp_count = lax.axis_size("tp")
    chips = tp_count // 2
    lanes = 128
    blocks = block_rows // lanes
    scores = route_score.astype(F32)
    weights = (scores / jnp.sum(scores, axis=1, keepdims=True) * ROUTED_SCALE).T
    named = routes.T
    column = named % tp_count
    place = jnp.where(column % 2 == core, 0, ep_count) + named // tp_count
    place = jnp.where(column // 2 == chip, place, -1)
    places = 2 * ep_count
    hit = place[:, None, :] == lax.broadcasted_iota(jnp.int32, (1, places, 1), 1)
    taken = jnp.any(hit, axis=0).astype(BF16)
    within = jnp.dot(
        taken.reshape(places * blocks, lanes), strict_upper(lanes), preferred_element_type=F32
    ).reshape(places, blocks, lanes)
    sums = jnp.sum(taken.reshape(places, blocks, lanes).astype(F32), axis=2).astype(BF16)
    ahead = jnp.dot(sums, strict_upper(blocks), preferred_element_type=F32)
    before = (within + ahead[:, :, None]).reshape(1, places, block_rows)
    rank = jnp.sum(jnp.where(hit, before, 0.0), axis=1).astype(jnp.int32)
    slot = jnp.where(place >= 0, place * capacity + rank, -1)

    def own_rows(table):
        mine = lax.dynamic_index_in_dim(
            table.reshape(top_count, chips, 2, lanes), core, axis=2, keepdims=False
        )
        doubled = jnp.concatenate([mine, mine], axis=1)
        turned = lax.dynamic_slice_in_dim(doubled, chip, chips, axis=1)
        return jnp.concatenate([turned[:, d] for d in ring_visits(chips)], axis=1)

    slot, weights = own_rows(slot), own_rows(weights)
    slots = places * capacity
    pick = jnp.zeros((slots, slot.shape[1]), jnp.bool_)
    down = lax.broadcasted_iota(jnp.int32, pick.shape, 0)
    for k in range(top_count):
        pick = pick | (down == slot[k][None, :])
    early = 3 * lanes
    spread = []
    for rows in (slice(0, early), slice(early, None)):
        part = jnp.zeros((slot[0, rows].shape[0], slots), F32)
        across = lax.broadcasted_iota(jnp.int32, part.shape, 1)
        for k in range(top_count):
            hit = across == slot[k, rows][:, None]
            part = part + jnp.where(hit, weights[k, rows][:, None], 0.0)
        spread.append(part.astype(BF16))
    return pick.astype(BF16), spread


def padded_rows(arrays, rows):
    height = sum(a.shape[0] for a in arrays)
    filler = jnp.zeros((rows - height, arrays[0].shape[1]), arrays[0].dtype)
    return jnp.concatenate([*arrays, filler], axis=0)


def shards(
    mix_in,
    mix_gain,
    mix_w_in,
    pool_mat,
    pool_scale,
    mix_w_out,
    moe_in,
    moe_gain,
    routes,
    route_score,
    exp_gate,
    exp_up,
    exp_down,
    shared_gate,
    shared_up,
    shared_down,
):
    tokens, width = moe_in.shape
    ep_count = lax.axis_size("ep")
    tp_count = lax.axis_size("tp")
    tp_index = lax.axis_index("tp")
    chip, core = tp_index // 2, tp_index % 2
    chips = tp_count // 2
    block_rows, top_count = routes.shape
    capacity = 2 * block_rows * top_count // (ep_count * tp_count)
    slots = ep_count * capacity
    half = width // 2

    normed = rms_rows(moe_in, moe_gain)
    pieces = [ring_gather(normed[:, f * half : (f + 1) * half]) for f in (0, 1)]

    routes, route_score = after(routes, normed), after(route_score, normed)
    pick, spread = slot_tables(routes, route_score, chip, core, capacity)
    for_own, from_other, shared_act = [], [], None
    rows_of = []
    for f in (0, 1):
        rows, for_other = select_rows(pick[slots:], pieces[f])
        from_other.append(to_partner(for_other))
        for_own.append(jnp.dot(pick[:slots], rows, preferred_element_type=F32).astype(BF16))
        rows_of.append(rows)
    outgoing = joined_sums(for_own, from_other)
    arrived = exchanged(outgoing.reshape(ep_count, capacity, width))
    arrived = arrived.reshape(slots, width)

    shared_gate, shared_up, shared_down = lax.optimization_barrier(
        (shared_gate, shared_up, shared_down, for_own[1])
    )[:3]
    shared_own = jnp.concatenate([shared_gate, shared_up, shared_down], axis=0)
    shared_other = to_partner(shared_own)
    units = shared_gate.shape[0]
    unit_rows = 128
    shared_in = jnp.concatenate(
        [
            padded_rows((shared_gate, shared_other[:units]), unit_rows),
            padded_rows((shared_up, shared_other[units : 2 * units]), unit_rows),
        ],
        axis=0,
    )
    shared_out = padded_rows((shared_down, shared_other[2 * units :]), unit_rows)

    for f in (0, 1):
        part = lax.dot_general(
            rows_of[f],
            shared_in[:, f * half : (f + 1) * half],
            (((1,), (1,)), ((), ())),
            preferred_element_type=F32,
        )
        shared_act = part if shared_act is None else shared_act + part
    shared_hidden = (
        jax.nn.silu(shared_act[:, :unit_rows]) * shared_act[:, unit_rows:]
    ).astype(BF16)

    arrived = after(arrived, shared_hidden)
    gate_act = jnp.dot(arrived, exp_gate[0], preferred_element_type=F32)
    up_act = jnp.dot(arrived, exp_up[0], preferred_element_type=F32)
    hidden = (jax.nn.silu(gate_act) * up_act).astype(BF16)
    results = jnp.dot(hidden, exp_down[0], preferred_element_type=F32).astype(BF16)

    out_blocks = jnp.concatenate(
        [mix_w_out[r : r + tokens] for r in range(0, mix_w_out.shape[0], tokens)], axis=1
    )
    mix_own = jnp.concatenate([mix_w_in, out_blocks], axis=1)
    mix_own = after(mix_own, *pieces[1][chips // 2])
    mix_flat = []
    for piece in ring_gather(mix_own):
        mix_flat.extend(piece if isinstance(piece, tuple) else (piece,))
    mix_pieces = stack_rows(mix_flat)
    mix_others = to_partner(mix_pieces)

    own = exchanged(results.reshape(ep_count, capacity, width))
    own = own.reshape(slots, width)
    other = to_partner(own)
    totals = []
    for part, (start, stop) in enumerate(((0, 3), (3, chips))):
        total = jnp.dot(
            shared_hidden[start * tokens : stop * tokens],
            shared_out,
            preferred_element_type=F32,
        )
        total += jnp.dot(spread[part][:, :slots], own, preferred_element_type=F32)
        total = lax.optimization_barrier(total)
        total += jnp.dot(spread[part][:, slots:], other, preferred_element_type=F32)
        totals.append(total.astype(BF16))
    strip = tokens // 2
    moe_out = last_sums(totals[1], [ring_scatter(totals, h, strip) for h in (0, 1)], strip)

    channels = mix_w_in.shape[1]
    position = jnp.stack([chip, core])
    mix_normed = rms_rows(after(mix_in, results), mix_gain)
    projected = project_rows(position, mix_normed, mix_pieces, mix_others, channels)
    reach_rows = 2 ** pool_mat.shape[0] - 1
    seq_len = tokens * ep_count * tp_count // SEQS_MIX
    first_row = lax.axis_index(("ep", "tp")) * tokens
    tail = shifted(projected[tokens - reach_rows :], ("ep", "tp"), 1)
    prior_tail = jnp.where(first_row % seq_len == 0, jnp.zeros_like(tail), tail)
    pool_out = pool_mix(projected, prior_tail, first_row, seq_len, pool_mat, pool_scale)
    mixed = output_rows(position, pool_out, mix_pieces, mix_others)
    return (mixed, moe_out)


def solution(mesh):
    return jax.shard_map(
        shards,
        mesh=mesh,
        in_specs=(
            P(("ep", "tp"), None),
            P(),
            P("tp", None),
            P(),
            P(),
            P(None, "tp"),
            P(("ep", "tp"), None),
            P(),
            P("ep", None),
            P("ep", None),
            P(("ep", "tp"), None, None),
            P(("ep", "tp"), None, None),
            P(("ep", "tp"), None, None),
            P("tp", None),
            P("tp", None),
            P("tp", None),
        ),
        out_specs=(P(("ep", "tp"), None), P(("ep", "tp"), None)),
        check_vma=False,
    )
```
